32 devices in a mesh: grp: 2 (over y), st: 4 (over z), tp: 4 (over x, core).
Axes of the slice: x: 2, y: 2, z: 4, core: 2. Of those that a mesh axis runs over, the one named last changes fastest.
Arguments:
- pass_ids: int32 [64, 4], P(('grp', 'st')), parts along dimension 0, may hold values from 0 to 63, as said below
- store: bfloat16 [64, 64, 2048], P('st', None, 'tp'), may hold values from -6 to 6
- queries: bfloat16 [8192, 1024], P(('grp', 'st'), 'tp'), parts along dimension 0, may hold values from -40 to 40
- gate_pre: bfloat16 [8192, 1024], P(('grp', 'st'), 'tp'), parts along dimension 0, may hold values from -6 to 6
- w_query: bfloat16 [2048, 1024], P(None, 'tp'), may hold values from -0.125 to 0.125
- w_gate: bfloat16 [2048, 1024], P(None, 'tp'), may hold values from -0.125 to 0.125
- w_key: bfloat16 [2048, 1024], P(None, 'tp'), may hold values from -0.125 to 0.125
- w_value: bfloat16 [2048, 1024], P(None, 'tp'), may hold values from -0.125 to 0.125
- d_mem: bfloat16 [8192, 1024], P(('grp', 'st'), 'tp'), parts along dimension 0, may hold values from -6 to 6
Outputs:
- d_tokens: bfloat16 [8192, 2048], P(('grp', 'st', 'tp')), parts along dimension 0
- d_store: bfloat16 [128, 64, 2048], P(('grp', 'st', 'tp')), parts along dimension 0
- d_wkey: float32 [4096, 1024], P(('grp', 'st'), 'tp'), parts along dimension 0
The draws below stay inside these ranges and needn't reach their ends.
There are 2 independent parts, one for each index of `grp`. The reference program is written for one: setup_inputs(seed, part) draws one part's arguments, and reference() takes and returns one part's arrays. A program takes and returns all parts, laid end to end along the dimension named above; an argument that names none is the same for every part. Nothing has to cross between parts.
Inputs may be any that keep to these rules, and one draw needn't show every extreme that they name: `pass_ids`: the 8 blocks of one index of st name at most 8 passages (counted with repetition) held by any one index of st o, that is passages o * 16 to o * 16 + 15. Every index of st takes exactly 8 passages from each of 4 indices of st and none from the others, so the bound 8 is reached by every index.
All inputs are finite; a program needn't handle non-finite values.
Results may differ from the reference program's by a relative error of at most 0.02.
Values may be sent and summed in bfloat16 or wider, within the bound.
A program may use at most 128 MiB of HBM per device.

```python
import jax
import jax.numpy as jnp
from jax import lax

D = 2048
HD = 256
MH = 4
BLK = 128
PB = 4
PL = 64
PASS_DEV = 16
MW = 1024
NBLK_DEV = 8
NBLK = 32
TOKENS = 4096
NPASS = 64
MOST = 8
N_ST = 4
N_TP = 4


def draw_pass_ids(key, part):
    folded = jax.random.fold_in(key, 17)
    key_hot, key_rank, key_order, key_pick, key_shift = jax.random.split(folded, 5)
    total_req = NBLK_DEV * PB
    used_owners = total_req // MOST
    device = jnp.arange(N_ST, dtype=jnp.int32)[:, None]
    owner_row = jnp.arange(N_ST, dtype=jnp.int32)[None, :]
    hottest = jax.random.randint(key_hot, (), 0, N_ST)
    levels = jnp.where(owner_row == hottest, 3, jnp.where(owner_row == (device - 1) % N_ST, 2, jnp.where(owner_row == (device + N_ST // 2) % N_ST, 1, 0)))
    jitter = jax.random.randint(key_rank, (N_ST, N_ST), 0, 1000)
    scores = levels * (1000 * N_ST) + jitter * N_ST + owner_row
    chosen = lax.top_k(scores, used_owners)[1].astype(jnp.int32)
    owners = jnp.repeat(chosen, MOST, axis=1)
    order_keys = jax.random.randint(key_order, (N_ST, total_req), 0, 1000) * total_req + jnp.arange(total_req, dtype=jnp.int32)[None, :]
    ordering = jnp.argsort(order_keys, axis=1)
    owners = jnp.take_along_axis(owners, ordering, axis=1)
    samples = jax.random.randint(key_pick, (3, N_ST, total_req), 0, PASS_DEV)
    popular = jnp.min(samples, axis=0)
    offsets = jax.random.randint(key_shift, (N_ST,), 0, PASS_DEV)
    within = (popular + offsets[owners]) % PASS_DEV
    passage_ids = owners * PASS_DEV + within
    return passage_ids.reshape(N_ST * NBLK_DEV, PB).astype(jnp.int32)


def draw_queries(key, part):
    folded = jax.random.fold_in(key, 23)
    key_base = jax.random.fold_in(folded, 0)
    base = jnp.clip(jax.random.normal(key_base, (TOKENS, MW), jnp.float32), -6.0, 6.0)
    return base.astype(jnp.bfloat16)


def level_of(own_key, dims, cuts, least, high):
    def one(dim, shards_of):
        steps = jax.random.uniform(jax.random.fold_in(jax.random.fold_in(own_key, 6), dim), (shards_of,), jnp.float32, least / len(cuts), high / len(cuts))
        return jnp.repeat(jnp.exp(steps), dims[dim] // shards_of).reshape((-1,) + (1,) * (len(dims) - dim - 1))

    loudness = one(*cuts[0])
    for cut in cuts[1:]:
        loudness = loudness * one(*cut)
    return loudness


def bell_draw(key, shape, deviation, reach, cuts=(), kind=jnp.bfloat16):
    array = jax.random.normal(key, shape, jnp.float32) * deviation
    if len(cuts) > 0:
        array = level_of(key, shape, cuts, -0.22, 0.18) * array
    return jnp.clip(array, min=-reach, max=reach).astype(kind)


def setup_inputs(seed: int = 0, part: int = 0) -> dict:
    keys = jax.random.split(jax.random.key(seed), 10)
    part_keys = jax.random.split(jax.random.fold_in(keys[9], part), 10)
    return {
        "pass_ids": draw_pass_ids(jax.random.fold_in(jax.random.fold_in(keys[9], part), 71), part),
        "store": bell_draw(keys[1], (NPASS, PL, D), 1.0, 6.0, ((0, 4), (2, 4))),
        "queries": draw_queries(jax.random.fold_in(jax.random.fold_in(keys[9], part), 71), part),
        "gate_pre": bell_draw(part_keys[3], (TOKENS, MW), 1.5, 6.0, ((0, 4), (1, 4))),
        "w_query": bell_draw(keys[4], (D, MW), D ** -0.5, 0.125, ((1, 4),)),
        "w_gate": bell_draw(keys[5], (D, MW), D ** -0.5, 0.125, ((1, 4),)),
        "w_key": bell_draw(keys[6], (D, MW), D ** -0.5, 0.125, ((1, 4),)),
        "w_value": bell_draw(keys[7], (D, MW), D ** -0.5, 0.125, ((1, 4),)),
        "d_mem": bell_draw(part_keys[8], (TOKENS, MW), 1.0, 6.0, ((0, 4), (1, 4))),
    }


def rounded_copy(values):
    return lax.optimization_barrier(values.astype(jnp.bfloat16)).astype(jnp.float32)


def reference(pass_ids, store, queries, gate_pre, w_query, w_gate, w_key, w_value, d_mem):
    flat_rows = store.reshape(NPASS * PL, D)
    keys_all = jnp.dot(flat_rows, w_key, preferred_element_type=jnp.float32).astype(jnp.bfloat16).reshape(NPASS, PL, MW)
    values_all = jnp.dot(flat_rows, w_value, preferred_element_type=jnp.float32).astype(jnp.bfloat16).reshape(NPASS, PL, MW)
    request_ids = pass_ids.reshape(-1).astype(jnp.int32)
    key_rows = keys_all[request_ids].reshape(NBLK, PB * PL, MH, HD).astype(jnp.float32)
    value_rows = values_all[request_ids].reshape(NBLK, PB * PL, MH, HD).astype(jnp.float32)
    query_rows = queries.reshape(NBLK, BLK, MH, HD).astype(jnp.float32)
    score_scale = HD ** -0.5
    scores = jnp.einsum('nqhd,nkhd->nhqk', query_rows, key_rows) * score_scale
    shifted = jnp.exp(scores - jnp.max(scores, axis=-1, keepdims=True))
    prob_rows = shifted / jnp.sum(shifted, axis=-1, keepdims=True)
    probs_low = rounded_copy(prob_rows)
    attended = jnp.einsum('nhqk,nkhd->nqhd', probs_low, value_rows).reshape(TOKENS, MW)
    gate_vals = gate_pre.astype(jnp.float32)
    sigmoid_vals = jax.nn.sigmoid(gate_vals)
    mem_grad = d_mem.astype(jnp.float32)
    attended_grad = rounded_copy(gate_vals * sigmoid_vals * mem_grad)
    gate_grad = rounded_copy(mem_grad * attended * sigmoid_vals * (1.0 + gate_vals * (1.0 - sigmoid_vals)))
    attended_four = attended_grad.reshape(NBLK, BLK, MH, HD)
    prob_grad = jnp.einsum('nqhd,nkhd->nhqk', attended_four, value_rows)
    score_grad = rounded_copy(score_scale * prob_rows * (prob_grad - jnp.sum(prob_rows * prob_grad, axis=-1, keepdims=True)))
    query_grad = rounded_copy(jnp.einsum('nhqk,nkhd->nqhd', score_grad, key_rows).reshape(TOKENS, MW))
    key_grad = rounded_copy(jnp.einsum('nhqk,nqhd->nkhd', score_grad, query_rows)).reshape(NBLK * PB, PL, MW)
    value_grad = rounded_copy(jnp.einsum('nhqk,nqhd->nkhd', probs_low, attended_four)).reshape(NBLK * PB, PL, MW)
    key_sums = jax.ops.segment_sum(key_grad, request_ids, NPASS).astype(jnp.bfloat16).reshape(NPASS * PL, MW)
    value_sums = jax.ops.segment_sum(value_grad, request_ids, NPASS).astype(jnp.bfloat16).reshape(NPASS * PL, MW)
    d_wkey = jnp.dot(flat_rows.T, key_sums, preferred_element_type=jnp.float32)
    group_width = MW // N_TP
    query_low = query_grad.astype(jnp.bfloat16)
    gate_low = gate_grad.astype(jnp.bfloat16)
    store_total = jnp.zeros((NPASS * PL, D), jnp.float32)
    token_total = jnp.zeros((TOKENS, D), jnp.float32)
    for group_index in range(N_TP):
        col_low = group_index * group_width
        col_high = col_low + group_width
        store_part = jnp.dot(key_sums[:, col_low:col_high], w_key[:, col_low:col_high].T, preferred_element_type=jnp.float32)
        store_part = store_part + jnp.dot(value_sums[:, col_low:col_high], w_value[:, col_low:col_high].T, preferred_element_type=jnp.float32)
        store_total = store_total + rounded_copy(store_part)
        token_part = jnp.dot(query_low[:, col_low:col_high], w_query[:, col_low:col_high].T, preferred_element_type=jnp.float32)
        token_part = token_part + jnp.dot(gate_low[:, col_low:col_high], w_gate[:, col_low:col_high].T, preferred_element_type=jnp.float32)
        token_total = token_total + rounded_copy(token_part)
    d_store = store_total.astype(jnp.bfloat16).reshape(NPASS, PL, D)
    d_tokens = token_total.astype(jnp.bfloat16)
    return (d_tokens, d_store, d_wkey)
```

```python
import functools

import jax
import jax.numpy as jnp
from jax import lax
from jax.experimental import pallas as pl
from jax.experimental.pallas import tpu as pltpu
from jax.sharding import PartitionSpec as P

HD = 256
BLK = 128
PB = 4
BF = jnp.bfloat16
F32 = jnp.float32
MESH = pl.DeviceIdType.MESH
NT = (((1,), (1,)), ((), ()))
TN = (((0,), (0,)), ((), ()))


def dot(a, b, dims=(((1,), (0,)), ((), ()))):
    return lax.dot_general(a, b, dims, preferred_element_type=F32)


def remote(src, dst, send, recv, device):
    return pltpu.make_async_remote_copy(
        src_ref=src,
        dst_ref=dst,
        send_sem=send,
        recv_sem=recv,
        device_id=device,
        device_id_type=MESH,
    )


def tile_of(size, most):
    while size % most:
        most //= 2
    return most


def kernel(
    st_n, tp_n, depth, pass_len,
    slot_ref, req_ref, ask_ref, store_ref, q_hbm, g_hbm, wq_hbm, wg_hbm, wk_hbm, wv_hbm, m_hbm,
    tok_out, store_out, wkey_out,
    rows, wkv, wqg, q_v, g_v, m_v, acc, kv, ask_in, ask_s, out, inc, kvb, reqg, gboth, arr,
    hot, plow, dwp, dwr, tp_part, tp_pair, tp_send, tp_recv, sp_part, sp_pair, sp_send, sp_recv,
    lsem, gs, gr, zs, zr, ps, pr, xs, xr,
):
    st = lax.axis_index("st")
    tp = lax.axis_index("tp")
    hi_n = tp_n // 2
    hi, lo = tp // 2, tp % 2
    mate = {"tp": hi * 2 + 1 - lo}
    pass_rows, chunk = rows.shape[1], rows.shape[2]
    model = wqg.shape[0]
    cols = q_v.shape[1]
    heads = cols // HD
    tok_rows = q_v.shape[0]
    blocks = tok_rows // BLK
    blk_keys = PB * pass_len

    def local(i, src, dst):
        copy = pltpu.make_async_copy(src, dst, lsem.at[i])
        copy.start()
        return copy

    own_rows = local(0, store_ref, rows.at[tp])
    loads_kv = [
        local(1, wk_hbm, wkv.at[:, pl.ds(0, cols)]),
        local(2, wv_hbm, wkv.at[:, pl.ds(cols, cols)]),
    ]
    loads_q = [local(3, q_hbm, q_v), local(4, g_hbm, g_v), local(5, m_hbm, m_v)]
    loads_qg = [
        local(6, wq_hbm, wqg.at[:, pl.ds(0, cols)]),
        local(7, wg_hbm, wqg.at[:, pl.ds(cols, cols)]),
    ]

    barrier = pltpu.get_barrier_semaphore()

    def greet_st(d, c):
        pl.semaphore_signal(
            barrier, inc=1, device_id={"st": (st + d) % st_n}, device_id_type=MESH
        )
        return c

    lax.fori_loop(1, st_n, greet_st, 0)
    for d in range(1, tp_n):
        pl.semaphore_signal(
            barrier, inc=1, device_id={"tp": (tp + d) % tp_n}, device_id_type=MESH
        )
    pl.semaphore_wait(barrier, st_n - 1 + tp_n - 1)

    across = []
    for d in range(1, hi_n):
        h = (hi + d) % hi_n
        across.append(
            remote(store_ref, rows.at[tp], gs.at[0, h], gr.at[tp], {"tp": h * 2 + lo})
        )
        across[-1].start()
    beside = remote(store_ref, rows.at[tp], gs.at[1, hi], gr.at[tp], mate)
    beside.start()

    def z_copy(phase, src, dst, peer):
        return remote(src, dst, zs.at[phase, peer], zr.at[phase, st], {"st": peer})

    def z_wait(phase, src, dst, peer):
        remote(src, dst, zs.at[phase, peer], zr.at[phase, peer], {"st": peer}).wait_recv()

    def ask_send(d, c):
        peer = (st + d) % st_n
        z_copy(0, ask_ref.at[peer], ask_in.at[st], peer).start()
        return c

    lax.fori_loop(1, st_n, ask_send, 0)
    ask_in[st] = ask_ref[st]

    m_tile = tile_of(pass_rows, 256)

    def project(t, first):
        def step(i, c):
            r = pl.ds(pl.multiple_of(i * m_tile, m_tile), m_tile)
            part = dot(rows[t, r], wkv[pl.ds(pl.multiple_of(t * chunk, chunk), chunk), :])
            acc[r] = part if first else acc[r] + part
            return c

        lax.fori_loop(0, pass_rows // m_tile, step, 0)

    def g_wait(t):
        remote(store_ref, rows.at[t], gs.at[1, hi], gr.at[t], mate).wait_recv()

    own_rows.wait()
    for copy in loads_kv:
        copy.wait()
    project(tp, True)
    g_wait(hi * 2 + 1 - lo)
    project(hi * 2 + 1 - lo, False)

    def ask_wait(d, c):
        peer = (st + d) % st_n
        z_wait(0, ask_ref.at[peer], ask_in.at[peer], peer)
        return c

    lax.fori_loop(1, st_n, ask_wait, 0)
    ask_copy = local(8, ask_in, ask_s)
    ask_copy.wait()

    hot_cols = depth * pass_len

    def hot_step(o, c):
        target = ask_in[o][0:1, :hot_cols]
        for i in range(pass_rows // m_tile):
            line = lax.broadcasted_iota(jnp.int32, (m_tile, hot_cols), 0) + i * m_tile
            hot[o, i * m_tile : (i + 1) * m_tile, :] = jnp.where(line == target, 1.0, 0.0).astype(BF)
        return c

    lax.fori_loop(0, st_n, hot_step, 0)
    onward = []
    for d in range(1, hi_n):
        h = (hi + d) % hi_n
        t = h * 2 + lo
        g_wait(t)
        onward.append(remote(rows.at[t], rows.at[t], gs.at[2, h], gr.at[t], mate))
        onward[-1].start()
        project(t, False)
    for d in range(1, hi_n):
        t = ((hi + d) % hi_n) * 2 + 1 - lo
        g_wait(t)
        project(t, False)

    def low_step(i, c):
        kv[i] = acc[pl.ds(pl.multiple_of(i * pass_len, pass_len), pass_len), :].astype(BF)
        return c

    lax.fori_loop(0, pass_rows // pass_len, low_step, 0)

    def kv_send(d, c):
        peer = (st + d) % st_n
        for k in range(depth):
            out[peer, k] = kv[ask_s[peer, 1, k]]
        z_copy(1, out.at[peer], inc.at[st], peer).start()
        return c

    lax.fori_loop(1, st_n, kv_send, 0)
    for k in range(depth):
        inc[st, k] = kv[ask_s[st, 1, k]]
    for copy in loads_q + loads_qg:
        copy.wait()

    def kv_wait(d, c):
        peer = (st + d) % st_n
        z_wait(1, out.at[peer], inc.at[peer], peer)
        return c

    lax.fori_loop(1, st_n, kv_wait, 0)

    scale = HD ** (-0.5)

    def block_step(b, c):
        r = pl.ds(pl.multiple_of(b * BLK, BLK), BLK)
        for j in range(PB):
            kvb[j * pass_len : (j + 1) * pass_len, :] = inc[
                slot_ref[0, b * PB + j], slot_ref[1, b * PB + j]
            ]
        for head in range(heads):
            hs = slice(head * HD, (head + 1) * HD)
            vs = slice(cols + head * HD, cols + (head + 1) * HD)
            q = q_v[r, hs]
            key = kvb[:, hs]
            value = kvb[:, vs]
            gate = g_v[r, hs].astype(F32)
            grad = m_v[r, hs].astype(F32)
            scores = dot(q, key, NT) * scale
            shifted = jnp.exp(scores - jnp.max(scores, axis=-1, keepdims=True))
            prob = shifted / jnp.sum(shifted, axis=-1, keepdims=True)
            low = prob.astype(BF)
            attended = dot(low, value)
            sig = 1.0 / (1.0 + jnp.exp(-gate))
            att_grad = (gate * sig * grad).astype(BF)
            gboth[r, vs] = (grad * attended * sig * (1.0 + gate * (1.0 - sig))).astype(BF)
            prob_grad = dot(att_grad, value, NT)
            inner = jnp.sum(prob * prob_grad, axis=-1, keepdims=True)
            score_grad = (scale * prob * (prob_grad - inner)).astype(BF)
            gboth[r, hs] = dot(score_grad, key).astype(BF)
            key_grad = dot(score_grad, q, TN).astype(BF)
            value_grad = dot(low, att_grad, TN).astype(BF)
            for j in range(PB):
                js = slice(j * pass_len, (j + 1) * pass_len)
                reqg[b * PB + j, :, hs] = key_grad[js]
                reqg[b * PB + j, :, vs] = value_grad[js]
        return c

    lax.fori_loop(0, blocks, block_step, 0)

    def grad_send(d, c):
        peer = (st + d) % st_n
        z_copy(1, out.at[peer], inc.at[st], peer).wait_send()
        for k in range(depth):
            out[peer, k] = reqg[req_ref[peer, k]]
        z_copy(2, out.at[peer], arr.at[st], peer).start()
        return c

    lax.fori_loop(1, st_n, grad_send, 0)
    for k in range(depth):
        arr[st, k] = reqg[req_ref[st, k]]

    n_tile = tile_of(model, 512)

    def expand(src, weight, part, pair_rows, t):
        base = pl.multiple_of(t * pair_rows, pair_rows)
        a = src[pl.ds(base, pair_rows), :]

        def step(i, c):
            n = pl.ds(pl.multiple_of(i * n_tile, n_tile), n_tile)
            part[t, :, n] = dot(a, weight[n, :], NT).astype(BF)
            return c

        lax.fori_loop(0, model // n_tile, step, 0)

    def pair_copy(which, part, pair, h):
        return remote(part.at[h * 2 + 1 - lo], pair.at[h], ps.at[which, h], pr.at[which, h], mate)

    def scatter_first(which, src, weight, part, pair, pair_rows):
        for d in range(1, hi_n + 1):
            h = (hi + d) % hi_n
            expand(src, weight, part, pair_rows, h * 2 + 1 - lo)
            pair_copy(which, part, pair, h).start()

    def cross(which, send, recv, h):
        return remote(
            send.at[h], recv.at[hi], xs.at[which, h], xr.at[which, hi], {"tp": h * 2 + lo}
        )

    def scatter_second(which, src, weight, part, pair, send, recv, pair_rows):
        for d in range(1, hi_n + 1):
            h = (hi + d) % hi_n
            expand(src, weight, part, pair_rows, h * 2 + lo)
            pair_copy(which, part, pair, h).wait_recv()
            if d < hi_n:
                send[h] = (part[h * 2 + lo].astype(F32) + pair[h].astype(F32)).astype(BF)
                cross(which, send, recv, h).start()

    def scatter_last(which, part, pair, send, recv, result):
        for d in range(1, hi_n):
            h = (hi + d) % hi_n
            remote(
                send.at[h], recv.at[h], xs.at[which, h], xr.at[which, h], {"tp": h * 2 + lo}
            ).wait_recv()
        total = part[tp].astype(F32) + pair[hi].astype(F32)
        for d in range(1, hi_n):
            total = total + recv[(hi + d) % hi_n].astype(F32)
        result[...] = total.astype(BF)

    tok_pair = tok_rows // tp_n
    sto_pair = pass_rows // tp_n
    scatter_first(0, gboth, wqg, tp_part, tp_pair, tok_pair)
    scatter_second(0, gboth, wqg, tp_part, tp_pair, tp_send, tp_recv, tok_pair)

    def grad_wait(d, c):
        peer = (st + d) % st_n
        z_wait(2, out.at[peer], arr.at[peer], peer)
        return c

    lax.fori_loop(1, st_n, grad_wait, 0)

    def sum_step(i, c):
        r = pl.ds(pl.multiple_of(i * m_tile, m_tile), m_tile)

        def owner(o, total):
            return total + dot(hot[o, r, :], arr[o].reshape(hot_cols, 2 * cols))

        total = lax.fori_loop(0, st_n, owner, jnp.zeros((m_tile, 2 * cols), F32))
        plow[r] = total.astype(BF)
        return c

    lax.fori_loop(0, pass_rows // m_tile, sum_step, 0)

    scatter_first(1, plow, wkv, sp_part, sp_pair, sto_pair)

    def wkey_step(t, c):
        dwp[pl.ds(pl.multiple_of(t * chunk, chunk), chunk), :] = dot(
            rows[t], plow[:, :cols], TN
        ).astype(BF)
        return c

    lax.fori_loop(0, tp_n, wkey_step, 0)
    share = model // st_n

    def part_of(s):
        return dwp.at[pl.ds(pl.multiple_of(s * share, share), share), :]

    def wkey_send(d, c):
        peer = (st + d) % st_n
        z_copy(3, part_of(peer), dwr.at[st], peer).start()
        return c

    lax.fori_loop(1, st_n, wkey_send, 0)
    scatter_second(1, plow, wkv, sp_part, sp_pair, sp_send, sp_recv, sto_pair)
    scatter_last(0, tp_part, tp_pair, tp_send, tp_recv, tok_out)
    wkey_out[...] = part_of(st)[...].astype(F32)

    def wkey_wait(d, c):
        peer = (st + d) % st_n
        z_wait(3, part_of(peer), dwr.at[peer], peer)
        wkey_out[...] += dwr[peer].astype(F32)
        return c

    lax.fori_loop(1, st_n, wkey_wait, 0)
    scatter_last(1, sp_part, sp_pair, sp_send, sp_recv, store_out)

    for copy in across + [beside] + onward:
        copy.wait_send()

    def drain(d, c):
        peer = (st + d) % st_n
        z_copy(0, ask_ref.at[peer], ask_in.at[st], peer).wait_send()
        z_copy(2, out.at[peer], arr.at[st], peer).wait_send()
        z_copy(3, part_of(peer), dwr.at[st], peer).wait_send()
        return c

    lax.fori_loop(1, st_n, drain, 0)
    for d in range(1, hi_n + 1):
        h = (hi + d) % hi_n
        pair_copy(0, tp_part, tp_pair, h).wait_send()
        pair_copy(1, sp_part, sp_pair, h).wait_send()
        if d < hi_n:
            cross(0, tp_send, tp_recv, h).wait_send()
            cross(1, sp_send, sp_recv, h).wait_send()


def local(pass_ids, store, queries, gate_pre, w_query, w_gate, w_key, w_value, d_mem):
    st_n = lax.axis_size("st")
    tp_n = lax.axis_size("tp")
    hi_n = tp_n // 2
    tok_rows, cols = queries.shape
    blocks = tok_rows // BLK
    passages, pass_len, chunk = store.shape
    model = w_key.shape[0]
    requests = blocks * PB
    depth = max(2, requests // st_n)
    pass_rows = passages * pass_len
    share = model // st_n

    ids = pass_ids.reshape(-1)
    owners = ids // passages
    within = ids % passages
    order = jnp.arange(requests, dtype=jnp.int32)
    earlier = (owners[None, :] == owners[:, None]) & (order[None, :] < order[:, None])
    rank = jnp.sum(earlier.astype(jnp.int32), axis=1)
    slots = jnp.stack([owners, rank])
    o_i = jnp.arange(st_n, dtype=jnp.int32)[:, None, None]
    k_i = jnp.arange(depth, dtype=jnp.int32)[None, :, None]
    match = (owners[None, None, :] == o_i) & (rank[None, None, :] == k_i)
    asked = jnp.max(jnp.where(match, within[None, None, :], -1), axis=2)
    req_of = jnp.max(jnp.where(match, order[None, None, :], 0), axis=2)
    hot_cols = depth * pass_len
    width = -(-hot_cols // 128) * 128
    lane = jnp.arange(width, dtype=jnp.int32)
    spread = jnp.repeat(asked, pass_len, axis=1)
    spread = jnp.pad(spread, ((0, 0), (0, width - hot_cols)), constant_values=-1)
    target = jnp.where(spread < 0, -1, spread * pass_len + lane[None, :] % pass_len)
    flat = jnp.pad(jnp.maximum(asked, 0), ((0, 0), (0, width - depth)))
    ask = jnp.concatenate(
        [target[:, None], flat[:, None], jnp.zeros((st_n, 6, width), jnp.int32)], axis=1
    )

    vmem = pl.BlockSpec(memory_space=pltpu.VMEM)
    smem = pl.BlockSpec(memory_space=pltpu.SMEM)
    hbm = pl.BlockSpec(memory_space=pl.ANY)
    V = pltpu.VMEM
    DMA = pltpu.SemaphoreType.DMA
    pair = 2 * cols
    tok_pair = tok_rows // tp_n
    sto_pair = pass_rows // tp_n
    d_tokens, d_store, d_wkey = pl.pallas_call(
        functools.partial(kernel, st_n, tp_n, depth, pass_len),
        out_shape=(
            jax.ShapeDtypeStruct((tok_pair, model), BF),
            jax.ShapeDtypeStruct((sto_pair, model), BF),
            jax.ShapeDtypeStruct((share, cols), F32),
        ),
        in_specs=[smem, smem, vmem] + [hbm] * 8,
        out_specs=(vmem, vmem, vmem),
        scratch_shapes=[
            V((tp_n, pass_rows, chunk), BF),
            V((model, pair), BF),
            V((model, pair), BF),
            V((tok_rows, cols), BF),
            V((tok_rows, cols), BF),
            V((tok_rows, cols), BF),
            V((pass_rows, pair), F32),
            V((passages, pass_len, pair), BF),
            V((st_n, 8, width), jnp.int32),
            pltpu.SMEM((st_n, 8, width), jnp.int32),
            V((st_n, depth, pass_len, pair), BF),
            V((st_n, depth, pass_len, pair), BF),
            V((PB * pass_len, pair), BF),
            V((requests, pass_len, pair), BF),
            V((tok_rows, pair), BF),
            V((st_n, depth, pass_len, pair), BF),
            V((st_n, pass_rows, hot_cols), BF),
            V((pass_rows, pair), BF),
            V((model, cols), BF),
            V((st_n, share, cols), BF),
            V((tp_n, tok_pair, model), BF),
            V((hi_n, tok_pair, model), BF),
            V((hi_n, tok_pair, model), BF),
            V((hi_n, tok_pair, model), BF),
            V((tp_n, sto_pair, model), BF),
            V((hi_n, sto_pair, model), BF),
            V((hi_n, sto_pair, model), BF),
            V((hi_n, sto_pair, model), BF),
            DMA((9,)),
            DMA((3, hi_n)),
            DMA((tp_n,)),
            DMA((4, st_n)),
            DMA((4, st_n)),
            DMA((2, hi_n)),
            DMA((2, hi_n)),
            DMA((2, hi_n)),
            DMA((2, hi_n)),
        ],
        compiler_params=pltpu.CompilerParams(
            collective_id=0, has_side_effects=True, vmem_limit_bytes=67043328
        ),
    )(
        slots, req_of, ask, store.reshape(pass_rows, chunk),
        queries, gate_pre, w_query, w_gate, w_key, w_value, d_mem,
    )
    return d_tokens, d_store.reshape(passages // tp_n, pass_len, model), d_wkey


def solution(mesh):
    return jax.shard_map(
        local,
        mesh=mesh,
        in_specs=(
            P(("grp", "st"), None),
            P("st", None, "tp"),
            P(("grp", "st"), "tp"),
            P(("grp", "st"), "tp"),
            P(None, "tp"),
            P(None, "tp"),
            P(None, "tp"),
            P(None, "tp"),
            P(("grp", "st"), "tp"),
        ),
        out_specs=(
            P(("grp", "st", "tp"), None),
            P(("grp", "st", "tp"), None, None),
            P(("grp", "st"), "tp"),
        ),
        check_vma=False,
    )
```

```python
import functools

import jax
import jax.numpy as jnp
from jax import lax
from jax.experimental import pallas as pl
from jax.experimental.pallas import tpu as pltpu
from jax.sharding import PartitionSpec as P

HD = 256
BLK = 128
PB = 4
BF = jnp.bfloat16
F32 = jnp.float32
MESH = pl.DeviceIdType.MESH
NT = (((1,), (1,)), ((), ()))
TN = (((0,), (0,)), ((), ()))


def dot(a, b, dims=(((1,), (0,)), ((), ()))):
    return lax.dot_general(a, b, dims, preferred_element_type=F32)


def remote(src, dst, send, recv, device):
    return pltpu.make_async_remote_copy(
        src_ref=src,
        dst_ref=dst,
        send_sem=send,
        recv_sem=recv,
        device_id=device,
        device_id_type=MESH,
    )


def tile_of(size, most):
    while size % most:
        most //= 2
    return most


def kernel(
    st_n, tp_n, depth, pass_len,
    slot_ref, req_ref, ask_ref, store_ref, q_hbm, g_hbm, wq_hbm, wg_hbm, wk_hbm, wv_hbm, m_hbm,
    tok_out, store_out, wkey_out,
    rows, wkv, wqg, q_v, g_v, m_v, acc, kv, ask_in, ask_s, out, inc, kvb, reqg, gboth, arr,
    hot, plow, dwp, dwr, tp_part, tp_pair, tp_send, tp_recv, sp_part, sp_pair, sp_send, sp_recv,
    lsem, gs, gr, zs, zr, ps, pr, xs, xr,
):
    st = lax.axis_index("st")
    tp = lax.axis_index("tp")
    hi_n = tp_n // 2
    hi, lo = tp // 2, tp % 2
    mate = {"tp": hi * 2 + 1 - lo}
    pass_rows, chunk = rows.shape[1], rows.shape[2]
    model = wqg.shape[0]
    cols = q_v.shape[1]
    heads = cols // HD
    tok_rows = q_v.shape[0]
    blocks = tok_rows // BLK
    blk_keys = PB * pass_len

    def local(i, src, dst):
        copy = pltpu.make_async_copy(src, dst, lsem.at[i])
        copy.start()
        return copy

    own_rows = local(0, store_ref, rows.at[tp])
    loads_kv = [
        local(1, wk_hbm, wkv.at[:, pl.ds(0, cols)]),
        local(2, wv_hbm, wkv.at[:, pl.ds(cols, cols)]),
    ]
    loads_q = [local(3, q_hbm, q_v), local(4, g_hbm, g_v), local(5, m_hbm, m_v)]
    loads_qg = [
        local(6, wq_hbm, wqg.at[:, pl.ds(0, cols)]),
        local(7, wg_hbm, wqg.at[:, pl.ds(cols, cols)]),
    ]

    barrier = pltpu.get_barrier_semaphore()

    def greet_st(d, c):
        pl.semaphore_signal(
            barrier, inc=1, device_id={"st": (st + d) % st_n}, device_id_type=MESH
        )
        return c

    lax.fori_loop(1, st_n, greet_st, 0)
    for d in range(1, tp_n):
        pl.semaphore_signal(
            barrier, inc=1, device_id={"tp": (tp + d) % tp_n}, device_id_type=MESH
        )
    pl.semaphore_wait(barrier, st_n - 1 + tp_n - 1)

    across = []
    for d in range(1, hi_n):
        h = (hi + d) % hi_n
        across.append(
            remote(store_ref, rows.at[tp], gs.at[0, h], gr.at[tp], {"tp": h * 2 + lo})
        )
        across[-1].start()
    beside = remote(store_ref, rows.at[tp], gs.at[1, hi], gr.at[tp], mate)
    beside.start()

    upper = st >= st_n // 2
    mark = jnp.where(upper, st, st_n - 1 - st)

    def far_peer(d):
        i = d - 1
        i = i + jnp.where(i >= mark, 1, 0)
        return jnp.where(upper, i, st_n - 1 - i)

    def z_copy(phase, src, dst, peer):
        return remote(src, dst, zs.at[phase, peer], zr.at[phase, st], {"st": peer})

    def z_wait(phase, src, dst, peer):
        remote(src, dst, zs.at[phase, peer], zr.at[phase, peer], {"st": peer}).wait_recv()

    def ask_send(d, c):
        peer = (st + d) % st_n
        z_copy(0, ask_ref.at[peer], ask_in.at[st], peer).start()
        return c

    lax.fori_loop(1, st_n, ask_send, 0)
    ask_in[st] = ask_ref[st]

    m_tile = tile_of(pass_rows, 256)

    def project(t, first):
        def step(i, c):
            r = pl.ds(pl.multiple_of(i * m_tile, m_tile), m_tile)
            part = dot(rows[t, r], wkv[pl.ds(pl.multiple_of(t * chunk, chunk), chunk), :])
            acc[r] = part if first else acc[r] + part
            return c

        lax.fori_loop(0, pass_rows // m_tile, step, 0)

    def g_wait(t):
        remote(store_ref, rows.at[t], gs.at[1, hi], gr.at[t], mate).wait_recv()

    own_rows.wait()
    for copy in loads_kv:
        copy.wait()
    project(tp, True)
    g_wait(hi * 2 + 1 - lo)
    project(hi * 2 + 1 - lo, False)

    def ask_wait(d, c):
        peer = (st + d) % st_n
        z_wait(0, ask_ref.at[peer], ask_in.at[peer], peer)
        return c

    lax.fori_loop(1, st_n, ask_wait, 0)
    ask_copy = local(8, ask_in, ask_s)
    ask_copy.wait()

    hot_cols = depth * pass_len

    def hot_step(o, c):
        target = ask_in[o][0:1, :hot_cols]
        for i in range(pass_rows // m_tile):
            line = lax.broadcasted_iota(jnp.int32, (m_tile, hot_cols), 0) + i * m_tile
            hot[o, i * m_tile : (i + 1) * m_tile, :] = jnp.where(line == target, 1.0, 0.0).astype(BF)
        return c

    lax.fori_loop(0, st_n, hot_step, 0)
    onward = []
    for d in range(1, hi_n):
        h = (hi + d) % hi_n
        t = h * 2 + lo
        g_wait(t)
        onward.append(remote(rows.at[t], rows.at[t], gs.at[2, h], gr.at[t], mate))
        onward[-1].start()
        project(t, False)
    for d in range(1, hi_n):
        t = ((hi + d) % hi_n) * 2 + 1 - lo
        g_wait(t)
        project(t, False)

    def low_step(i, c):
        kv[i] = acc[pl.ds(pl.multiple_of(i * pass_len, pass_len), pass_len), :].astype(BF)
        return c

    lax.fori_loop(0, pass_rows // pass_len, low_step, 0)

    def kv_send(d, c):
        peer = far_peer(d)
        for k in range(depth):
            out[peer, k] = kv[ask_s[peer, 1, k]]
        z_copy(1, out.at[peer], inc.at[st], peer).start()
        return c

    lax.fori_loop(1, st_n, kv_send, 0)
    for k in range(depth):
        inc[st, k] = kv[ask_s[st, 1, k]]
    for copy in loads_q + loads_qg:
        copy.wait()

    def kv_wait(d, c):
        peer = (st + d) % st_n
        z_wait(1, out.at[peer], inc.at[peer], peer)
        return c

    lax.fori_loop(1, st_n, kv_wait, 0)

    scale = HD ** (-0.5)

    def block_step(b, c):
        r = pl.ds(pl.multiple_of(b * BLK, BLK), BLK)
        for j in range(PB):
            kvb[j * pass_len : (j + 1) * pass_len, :] = inc[
                slot_ref[0, b * PB + j], slot_ref[1, b * PB + j]
            ]
        for head in range(heads):
            hs = slice(head * HD, (head + 1) * HD)
            vs = slice(cols + head * HD, cols + (head + 1) * HD)
            q = q_v[r, hs]
            key = kvb[:, hs]
            value = kvb[:, vs]
            gate = g_v[r, hs].astype(F32)
            grad = m_v[r, hs].astype(F32)
            scores = dot(q, key, NT) * scale
            shifted = jnp.exp(scores - jnp.max(scores, axis=-1, keepdims=True))
            prob = shifted / jnp.sum(shifted, axis=-1, keepdims=True)
            low = prob.astype(BF)
            attended = dot(low, value)
            sig = 1.0 / (1.0 + jnp.exp(-gate))
            att_grad = (gate * sig * grad).astype(BF)
            gboth[r, vs] = (grad * attended * sig * (1.0 + gate * (1.0 - sig))).astype(BF)
            prob_grad = dot(att_grad, value, NT)
            inner = jnp.sum(prob * prob_grad, axis=-1, keepdims=True)
            score_grad = (scale * prob * (prob_grad - inner)).astype(BF)
            gboth[r, hs] = dot(score_grad, key).astype(BF)
            key_grad = dot(score_grad, q, TN).astype(BF)
            value_grad = dot(low, att_grad, TN).astype(BF)
            for j in range(PB):
                js = slice(j * pass_len, (j + 1) * pass_len)
                reqg[b * PB + j, :, hs] = key_grad[js]
                reqg[b * PB + j, :, vs] = value_grad[js]
        return c

    lax.fori_loop(0, blocks, block_step, 0)

    def grad_send(d, c):
        peer = far_peer(d)
        z_copy(1, out.at[peer], inc.at[st], peer).wait_send()
        for k in range(depth):
            out[peer, k] = reqg[req_ref[peer, k]]
        z_copy(2, out.at[peer], arr.at[st], peer).start()
        return c

    lax.fori_loop(1, st_n, grad_send, 0)
    for k in range(depth):
        arr[st, k] = reqg[req_ref[st, k]]

    n_tile = tile_of(model, 512)

    def expand(src, weight, part, pair_rows, t):
        base = pl.multiple_of(t * pair_rows, pair_rows)
        a = src[pl.ds(base, pair_rows), :]

        def step(i, c):
            n = pl.ds(pl.multiple_of(i * n_tile, n_tile), n_tile)
            part[t, :, n] = dot(a, weight[n, :], NT).astype(BF)
            return c

        lax.fori_loop(0, model // n_tile, step, 0)

    def pair_copy(which, part, pair, h):
        return remote(part.at[h * 2 + 1 - lo], pair.at[h], ps.at[which, h], pr.at[which, h], mate)

    def scatter_first(which, src, weight, part, pair, pair_rows):
        for d in range(1, hi_n + 1):
            h = (hi + d) % hi_n
            expand(src, weight, part, pair_rows, h * 2 + 1 - lo)
            pair_copy(which, part, pair, h).start()

    def cross(which, send, recv, h):
        return remote(
            send.at[h], recv.at[hi], xs.at[which, h], xr.at[which, hi], {"tp": h * 2 + lo}
        )

    def scatter_second(which, src, weight, part, pair, send, recv, pair_rows):
        for d in range(1, hi_n + 1):
            h = (hi + d) % hi_n
            expand(src, weight, part, pair_rows, h * 2 + lo)
            pair_copy(which, part, pair, h).wait_recv()
            if d < hi_n:
                send[h] = (part[h * 2 + lo].astype(F32) + pair[h].astype(F32)).astype(BF)
                cross(which, send, recv, h).start()

    def scatter_last(which, part, pair, send, recv, result):
        for d in range(1, hi_n):
            h = (hi + d) % hi_n
            remote(
                send.at[h], recv.at[h], xs.at[which, h], xr.at[which, h], {"tp": h * 2 + lo}
            ).wait_recv()
        total = part[tp].astype(F32) + pair[hi].astype(F32)
        for d in range(1, hi_n):
            total = total + recv[(hi + d) % hi_n].astype(F32)
        result[...] = total.astype(BF)

    tok_pair = tok_rows // tp_n
    sto_pair = pass_rows // tp_n
    scatter_first(0, gboth, wqg, tp_part, tp_pair, tok_pair)
    scatter_second(0, gboth, wqg, tp_part, tp_pair, tp_send, tp_recv, tok_pair)

    def gather_sums(o, first):
        def step(i, c):
            r = pl.ds(pl.multiple_of(i * m_tile, m_tile), m_tile)
            part = dot(hot[o, r, :], arr[o].reshape(hot_cols, 2 * cols))
            acc[r] = part if first else acc[r] + part
            return c

        lax.fori_loop(0, pass_rows // m_tile, step, 0)

    gather_sums(st, True)

    def grad_wait(d, c):
        peer = (st + d) % st_n
        z_wait(2, out.at[peer], arr.at[peer], peer)
        gather_sums(peer, False)
        return c

    lax.fori_loop(1, st_n, grad_wait, 0)
    plow[...] = acc[...].astype(BF)

    scatter_first(1, plow, wkv, sp_part, sp_pair, sto_pair)

    def wkey_step(t, c):
        dwp[pl.ds(pl.multiple_of(t * chunk, chunk), chunk), :] = dot(
            rows[t], plow[:, :cols], TN
        ).astype(BF)
        return c

    lax.fori_loop(0, tp_n, wkey_step, 0)
    share = model // st_n

    def part_of(s):
        return dwp.at[pl.ds(pl.multiple_of(s * share, share), share), :]

    def wkey_send(d, c):
        peer = far_peer(d)
        z_copy(3, part_of(peer), dwr.at[st], peer).start()
        return c

    lax.fori_loop(1, st_n, wkey_send, 0)
    scatter_second(1, plow, wkv, sp_part, sp_pair, sp_send, sp_recv, sto_pair)
    scatter_last(0, tp_part, tp_pair, tp_send, tp_recv, tok_out)
    wkey_out[...] = part_of(st)[...].astype(F32)

    def wkey_wait(d, c):
        peer = (st + d) % st_n
        z_wait(3, part_of(peer), dwr.at[peer], peer)
        wkey_out[...] += dwr[peer].astype(F32)
        return c

    lax.fori_loop(1, st_n, wkey_wait, 0)
    scatter_last(1, sp_part, sp_pair, sp_send, sp_recv, store_out)

    for copy in across + [beside] + onward:
        copy.wait_send()

    def drain(d, c):
        peer = (st + d) % st_n
        z_copy(0, ask_ref.at[peer], ask_in.at[st], peer).wait_send()
        z_copy(2, out.at[peer], arr.at[st], peer).wait_send()
        z_copy(3, part_of(peer), dwr.at[st], peer).wait_send()
        return c

    lax.fori_loop(1, st_n, drain, 0)
    for d in range(1, hi_n + 1):
        h = (hi + d) % hi_n
        pair_copy(0, tp_part, tp_pair, h).wait_send()
        pair_copy(1, sp_part, sp_pair, h).wait_send()
        if d < hi_n:
            cross(0, tp_send, tp_recv, h).wait_send()
            cross(1, sp_send, sp_recv, h).wait_send()


def local(pass_ids, store, queries, gate_pre, w_query, w_gate, w_key, w_value, d_mem):
    st_n = lax.axis_size("st")
    tp_n = lax.axis_size("tp")
    hi_n = tp_n // 2
    tok_rows, cols = queries.shape
    blocks = tok_rows // BLK
    passages, pass_len, chunk = store.shape
    model = w_key.shape[0]
    requests = blocks * PB
    depth = max(2, requests // st_n)
    pass_rows = passages * pass_len
    share = model // st_n

    ids = pass_ids.reshape(-1)
    owners = ids // passages
    within = ids % passages
    order = jnp.arange(requests, dtype=jnp.int32)
    earlier = (owners[None, :] == owners[:, None]) & (order[None, :] < order[:, None])
    rank = jnp.sum(earlier.astype(jnp.int32), axis=1)
    slots = jnp.stack([owners, rank])
    o_i = jnp.arange(st_n, dtype=jnp.int32)[:, None, None]
    k_i = jnp.arange(depth, dtype=jnp.int32)[None, :, None]
    match = (owners[None, None, :] == o_i) & (rank[None, None, :] == k_i)
    asked = jnp.max(jnp.where(match, within[None, None, :], -1), axis=2)
    req_of = jnp.max(jnp.where(match, order[None, None, :], 0), axis=2)
    hot_cols = depth * pass_len
    width = -(-hot_cols // 128) * 128
    lane = jnp.arange(width, dtype=jnp.int32)
    spread = jnp.repeat(asked, pass_len, axis=1)
    spread = jnp.pad(spread, ((0, 0), (0, width - hot_cols)), constant_values=-1)
    target = jnp.where(spread < 0, -1, spread * pass_len + lane[None, :] % pass_len)
    flat = jnp.pad(jnp.maximum(asked, 0), ((0, 0), (0, width - depth)))
    ask = jnp.concatenate(
        [target[:, None], flat[:, None], jnp.zeros((st_n, 6, width), jnp.int32)], axis=1
    )

    vmem = pl.BlockSpec(memory_space=pltpu.VMEM)
    smem = pl.BlockSpec(memory_space=pltpu.SMEM)
    hbm = pl.BlockSpec(memory_space=pl.ANY)
    V = pltpu.VMEM
    DMA = pltpu.SemaphoreType.DMA
    pair = 2 * cols
    tok_pair = tok_rows // tp_n
    sto_pair = pass_rows // tp_n
    d_tokens, d_store, d_wkey = pl.pallas_call(
        functools.partial(kernel, st_n, tp_n, depth, pass_len),
        out_shape=(
            jax.ShapeDtypeStruct((tok_pair, model), BF),
            jax.ShapeDtypeStruct((sto_pair, model), BF),
            jax.ShapeDtypeStruct((share, cols), F32),
        ),
        in_specs=[smem, smem, vmem] + [hbm] * 8,
        out_specs=(vmem, vmem, vmem),
        scratch_shapes=[
            V((tp_n, pass_rows, chunk), BF),
            V((model, pair), BF),
            V((model, pair), BF),
            V((tok_rows, cols), BF),
            V((tok_rows, cols), BF),
            V((tok_rows, cols), BF),
            V((pass_rows, pair), F32),
            V((passages, pass_len, pair), BF),
            V((st_n, 8, width), jnp.int32),
            pltpu.SMEM((st_n, 8, width), jnp.int32),
            V((st_n, depth, pass_len, pair), BF),
            V((st_n, depth, pass_len, pair), BF),
            V((PB * pass_len, pair), BF),
            V((requests, pass_len, pair), BF),
            V((tok_rows, pair), BF),
            V((st_n, depth, pass_len, pair), BF),
            V((st_n, pass_rows, hot_cols), BF),
            V((pass_rows, pair), BF),
            V((model, cols), BF),
            V((st_n, share, cols), BF),
            V((tp_n, tok_pair, model), BF),
            V((hi_n, tok_pair, model), BF),
            V((hi_n, tok_pair, model), BF),
            V((hi_n, tok_pair, model), BF),
            V((tp_n, sto_pair, model), BF),
            V((hi_n, sto_pair, model), BF),
            V((hi_n, sto_pair, model), BF),
            V((hi_n, sto_pair, model), BF),
            DMA((9,)),
            DMA((3, hi_n)),
            DMA((tp_n,)),
            DMA((4, st_n)),
            DMA((4, st_n)),
            DMA((2, hi_n)),
            DMA((2, hi_n)),
            DMA((2, hi_n)),
            DMA((2, hi_n)),
        ],
        compiler_params=pltpu.CompilerParams(
            collective_id=0, has_side_effects=True, vmem_limit_bytes=67043328
        ),
    )(
        slots, req_of, ask, store.reshape(pass_rows, chunk),
        queries, gate_pre, w_query, w_gate, w_key, w_value, d_mem,
    )
    return d_tokens, d_store.reshape(passages // tp_n, pass_len, model), d_wkey


def solution(mesh):
    return jax.shard_map(
        local,
        mesh=mesh,
        in_specs=(
            P(("grp", "st"), None),
            P("st", None, "tp"),
            P(("grp", "st"), "tp"),
            P(("grp", "st"), "tp"),
            P(None, "tp"),
            P(None, "tp"),
            P(None, "tp"),
            P(None, "tp"),
            P(("grp", "st"), "tp"),
        ),
        out_specs=(
            P(("grp", "st", "tp"), None),
            P(("grp", "st", "tp"), None, None),
            P(("grp", "st"), "tp"),
        ),
        check_vma=False,
    )
```

```python
import functools

import jax
import jax.numpy as jnp
from jax import lax
from jax.experimental import pallas as pl
from jax.experimental.pallas import tpu as pltpu
from jax.sharding import PartitionSpec as P

HD = 256
BLK = 128
PB = 4
BF = jnp.bfloat16
F32 = jnp.float32
MESH = pl.DeviceIdType.MESH
NT = (((1,), (1,)), ((), ()))
TN = (((0,), (0,)), ((), ()))


def dot(a, b, dims=(((1,), (0,)), ((), ()))):
    return lax.dot_general(a, b, dims, preferred_element_type=F32)


def remote(src, dst, send, recv, device):
    return pltpu.make_async_remote_copy(
        src_ref=src,
        dst_ref=dst,
        send_sem=send,
        recv_sem=recv,
        device_id=device,
        device_id_type=MESH,
    )


def tile_of(size, most):
    while size % most:
        most //= 2
    return most


def kernel(
    st_n, tp_n, depth, pass_len,
    slot_ref, req_ref, ask_ref, store_ref, q_hbm, g_hbm, wq_hbm, wg_hbm, wk_hbm, wv_hbm, m_hbm,
    tok_out, store_out, wkey_out,
    rows, wkv, wqg, q_v, g_v, m_v, acc, kv, ask_in, ask_s, out, inc_k, inc_v, ret, prob_v, kvb, reqg, gboth, arr,
    hot, plow, dwp, dwr, tp_part, tp_pair, tp_recv, sp_part, sp_pair, sp_recv,
    lsem, gs, gr, zs, zr, ps, pr, xs, xr,
):
    st = lax.axis_index("st")
    tp = lax.axis_index("tp")
    hi_n = tp_n // 2
    hi, lo = tp // 2, tp % 2
    mate = {"tp": hi * 2 + 1 - lo}
    pass_rows, chunk = rows.shape[1], rows.shape[2]
    model = wqg.shape[0]
    cols = q_v.shape[1]
    heads = cols // HD
    tok_rows = q_v.shape[0]
    blocks = tok_rows // BLK
    blk_keys = PB * pass_len

    def local(i, src, dst):
        copy = pltpu.make_async_copy(src, dst, lsem.at[i])
        copy.start()
        return copy

    own_rows = local(0, store_ref, rows.at[tp])
    loads_kv = [
        local(1, wk_hbm, wkv.at[:, pl.ds(0, cols)]),
        local(2, wv_hbm, wkv.at[:, pl.ds(cols, cols)]),
    ]
    loads_q = [local(3, q_hbm, q_v), local(4, g_hbm, g_v), local(5, m_hbm, m_v)]
    loads_qg = [
        local(6, wq_hbm, wqg.at[:, pl.ds(0, cols)]),
        local(7, wg_hbm, wqg.at[:, pl.ds(cols, cols)]),
    ]

    barrier = pltpu.get_barrier_semaphore()

    def greet_st(d, c):
        pl.semaphore_signal(
            barrier, inc=1, device_id={"st": (st + d) % st_n}, device_id_type=MESH
        )
        return c

    lax.fori_loop(1, st_n, greet_st, 0)
    for d in range(1, tp_n):
        pl.semaphore_signal(
            barrier, inc=1, device_id={"tp": (tp + d) % tp_n}, device_id_type=MESH
        )
    pl.semaphore_wait(barrier, st_n - 1 + tp_n - 1)

    across = []
    for d in range(1, hi_n):
        h = (hi + d) % hi_n
        across.append(
            remote(store_ref, rows.at[tp], gs.at[0, h], gr.at[tp], {"tp": h * 2 + lo})
        )
        across[-1].start()
    beside = remote(store_ref, rows.at[tp], gs.at[1, hi], gr.at[tp], mate)
    beside.start()

    upper = st >= st_n // 2
    mark = jnp.where(upper, st, st_n - 1 - st)

    def far_peer(d):
        i = d - 1
        i = i + jnp.where(i >= mark, 1, 0)
        return jnp.where(upper, i, st_n - 1 - i)

    def z_copy(phase, src, dst, peer):
        return remote(src, dst, zs.at[phase, peer], zr.at[phase, st], {"st": peer})

    def z_wait(phase, src, dst, peer):
        remote(src, dst, zs.at[phase, peer], zr.at[phase, peer], {"st": peer}).wait_recv()

    def ask_send(d, c):
        peer = (st + d) % st_n
        z_copy(0, ask_ref.at[peer], ask_in.at[st], peer).start()
        return c

    lax.fori_loop(1, st_n, ask_send, 0)
    ask_in[st] = ask_ref[st]

    m_tile = tile_of(pass_rows, 256)

    def project(t, first):
        def step(i, c):
            r = pl.ds(pl.multiple_of(i * m_tile, m_tile), m_tile)
            part = dot(rows[t, r], wkv[pl.ds(pl.multiple_of(t * chunk, chunk), chunk), :])
            acc[r] = part if first else acc[r] + part
            return c

        lax.fori_loop(0, pass_rows // m_tile, step, 0)

    def g_wait(t):
        remote(store_ref, rows.at[t], gs.at[1, hi], gr.at[t], mate).wait_recv()

    own_rows.wait()
    for copy in loads_kv:
        copy.wait()
    project(tp, True)
    g_wait(hi * 2 + 1 - lo)
    project(hi * 2 + 1 - lo, False)

    def ask_wait(d, c):
        peer = (st + d) % st_n
        z_wait(0, ask_ref.at[peer], ask_in.at[peer], peer)
        return c

    lax.fori_loop(1, st_n, ask_wait, 0)
    ask_copy = local(8, ask_in, ask_s)
    ask_copy.wait()

    hot_cols = depth * pass_len

    def hot_step(o, c):
        target = ask_in[o][0:1, :hot_cols]
        for i in range(pass_rows // m_tile):
            line = lax.broadcasted_iota(jnp.int32, (m_tile, hot_cols), 0) + i * m_tile
            hot[o, i * m_tile : (i + 1) * m_tile, :] = jnp.where(line == target, 1.0, 0.0).astype(BF)
        return c

    lax.fori_loop(0, st_n, hot_step, 0)
    onward = []
    for d in range(1, hi_n):
        h = (hi + d) % hi_n
        t = h * 2 + lo
        g_wait(t)
        onward.append(remote(rows.at[t], rows.at[t], gs.at[2, h], gr.at[t], mate))
        onward[-1].start()
        project(t, False)
    for d in range(1, hi_n):
        t = ((hi + d) % hi_n) * 2 + 1 - lo
        g_wait(t)
        project(t, False)

    def low_step(i, c):
        kv[i] = acc[pl.ds(pl.multiple_of(i * pass_len, pass_len), pass_len), :].astype(BF)
        return c

    lax.fori_loop(0, pass_rows // pass_len, low_step, 0)

    ks, vs_all = pl.ds(0, cols), pl.ds(cols, cols)

    def half(ref, peer, part):
        return ref.at[peer, :, :, part]

    def key_copy(peer):
        return z_copy(1, half(out, peer, ks), inc_k.at[st], peer)

    def value_copy(peer):
        return z_copy(4, half(out, peer, vs_all), inc_v.at[st], peer)

    def kv_send(d, c):
        peer = far_peer(d)
        for k in range(depth):
            out[peer, k] = kv[ask_s[peer, 1, k]]
        key_copy(peer).start()
        return c

    def value_send(d, c):
        value_copy(far_peer(d)).start()
        return c

    lax.fori_loop(1, st_n, kv_send, 0)
    lax.fori_loop(1, st_n, value_send, 0)
    for k in range(depth):
        picked = kv[ask_s[st, 1, k]]
        inc_k[st, k] = picked[:, :cols]
        inc_v[st, k] = picked[:, cols:]
    for copy in loads_q + loads_qg:
        copy.wait()

    def key_wait(d, c):
        peer = (st + d) % st_n
        z_wait(1, half(out, peer, ks), inc_k.at[peer], peer)
        return c

    lax.fori_loop(1, st_n, key_wait, 0)
    scale = HD ** (-0.5)

    def probs_step(b, c):
        r = pl.ds(pl.multiple_of(b * BLK, BLK), BLK)
        for j in range(PB):
            kvb[j * pass_len : (j + 1) * pass_len, :cols] = inc_k[
                slot_ref[0, b * PB + j], slot_ref[1, b * PB + j]
            ]
        for head in range(heads):
            hs = slice(head * HD, (head + 1) * HD)
            vs = slice(cols + head * HD, cols + (head + 1) * HD)
            gate = g_v[r, hs].astype(F32)
            scores = dot(q_v[r, hs], kvb[:, hs], NT) * scale
            shifted = jnp.exp(scores - jnp.max(scores, axis=-1, keepdims=True))
            prob = shifted / jnp.sum(shifted, axis=-1, keepdims=True)
            prob_v[head, r, :] = prob
            sig = 1.0 / (1.0 + jnp.exp(-gate))
            att_grad = (gate * sig * m_v[r, hs].astype(F32)).astype(BF)
            value_grad = dot(prob.astype(BF), att_grad, TN).astype(BF)
            for j in range(PB):
                reqg[b * PB + j, :, vs] = value_grad[j * pass_len : (j + 1) * pass_len]
        return c

    lax.fori_loop(0, blocks, probs_step, 0)

    def back_copy(phase, part, peer):
        return z_copy(phase, half(ret, peer, part), half(arr, st, part), peer)

    def give_back(phase, part, span):
        def send(d, c):
            peer = far_peer(d)
            for k in range(depth):
                ret[peer, k, :, span] = reqg[req_ref[peer, k]][:, span]
            back_copy(phase, part, peer).start()
            return c

        lax.fori_loop(1, st_n, send, 0)
        for k in range(depth):
            arr[st, k, :, span] = reqg[req_ref[st, k]][:, span]

    give_back(2, vs_all, slice(cols, 2 * cols))

    def value_wait(d, c):
        peer = (st + d) % st_n
        z_wait(4, half(out, peer, vs_all), inc_v.at[peer], peer)
        return c

    lax.fori_loop(1, st_n, value_wait, 0)

    def block_step(b, c):
        r = pl.ds(pl.multiple_of(b * BLK, BLK), BLK)
        for j in range(PB):
            o, k = slot_ref[0, b * PB + j], slot_ref[1, b * PB + j]
            kvb[j * pass_len : (j + 1) * pass_len, :cols] = inc_k[o, k]
            kvb[j * pass_len : (j + 1) * pass_len, cols:] = inc_v[o, k]
        for head in range(heads):
            hs = slice(head * HD, (head + 1) * HD)
            vs = slice(cols + head * HD, cols + (head + 1) * HD)
            q = q_v[r, hs]
            key = kvb[:, hs]
            value = kvb[:, vs]
            gate = g_v[r, hs].astype(F32)
            grad = m_v[r, hs].astype(F32)
            prob = prob_v[head, r, :]
            attended = dot(prob.astype(BF), value)
            sig = 1.0 / (1.0 + jnp.exp(-gate))
            att_grad = (gate * sig * grad).astype(BF)
            gboth[r, vs] = (grad * attended * sig * (1.0 + gate * (1.0 - sig))).astype(BF)
            prob_grad = dot(att_grad, value, NT)
            inner = jnp.sum(prob * prob_grad, axis=-1, keepdims=True)
            score_grad = (scale * prob * (prob_grad - inner)).astype(BF)
            gboth[r, hs] = dot(score_grad, key).astype(BF)
            key_grad = dot(score_grad, q, TN).astype(BF)
            for j in range(PB):
                reqg[b * PB + j, :, hs] = key_grad[j * pass_len : (j + 1) * pass_len]
        return c

    lax.fori_loop(0, blocks, block_step, 0)
    give_back(5, ks, slice(0, cols))

    n_tile = tile_of(model, 512)

    def expand(src, weight, part, pair_rows, t):
        base = pl.multiple_of(t * pair_rows, pair_rows)
        a = src[pl.ds(base, pair_rows), :]

        def step(i, c):
            n = pl.ds(pl.multiple_of(i * n_tile, n_tile), n_tile)
            part[t, :, n] = dot(a, weight[n, :], NT).astype(BF)
            return c

        lax.fori_loop(0, model // n_tile, step, 0)

    def pair_copy(which, part, pair, h):
        return remote(part.at[h * 2 + 1 - lo], pair.at[h], ps.at[which, h], pr.at[which, h], mate)

    def scatter_first(which, src, weight, part, pair, pair_rows):
        for d in range(1, hi_n + 1):
            h = (hi + d) % hi_n
            expand(src, weight, part, pair_rows, h * 2 + 1 - lo)
            pair_copy(which, part, pair, h).start()

    def cross(which, send, recv, h):
        return remote(
            send.at[h * 2 + lo], recv.at[hi], xs.at[which, h], xr.at[which, hi], {"tp": h * 2 + lo}
        )

    def scatter_second(which, src, weight, part, pair, send, recv, pair_rows):
        for d in range(1, hi_n + 1):
            h = (hi + d) % hi_n
            expand(src, weight, part, pair_rows, h * 2 + lo)
            pair_copy(which, part, pair, h).wait_recv()
            if d < hi_n:
                part[h * 2 + lo] = (part[h * 2 + lo].astype(F32) + pair[h].astype(F32)).astype(BF)
                cross(which, part, recv, h).start()

    def scatter_last(which, part, pair, send, recv, result):
        for d in range(1, hi_n):
            h = (hi + d) % hi_n
            remote(
                send.at[h * 2 + lo], recv.at[h], xs.at[which, h], xr.at[which, h], {"tp": h * 2 + lo}
            ).wait_recv()
        total = part[tp].astype(F32) + pair[hi].astype(F32)
        for d in range(1, hi_n):
            total = total + recv[(hi + d) % hi_n].astype(F32)
        result[...] = total.astype(BF)

    tok_pair = tok_rows // tp_n
    sto_pair = pass_rows // tp_n
    scatter_first(0, gboth, wqg, tp_part, tp_pair, tok_pair)
    scatter_second(0, gboth, wqg, tp_part, tp_pair, tp_part, tp_recv, tok_pair)

    def gather_sums(o, span, first):
        def step(i, c):
            r = pl.ds(pl.multiple_of(i * m_tile, m_tile), m_tile)
            part = dot(hot[o, r, :], arr[o, :, :, span].reshape(hot_cols, cols))
            acc[r, span] = part if first else acc[r, span] + part
            return c

        lax.fori_loop(0, pass_rows // m_tile, step, 0)

    for phase, part, span in ((2, vs_all, slice(cols, 2 * cols)), (5, ks, slice(0, cols))):
        gather_sums(st, span, True)

        def grad_wait(d, c):
            peer = (st + d) % st_n
            z_wait(phase, half(ret, peer, part), half(arr, peer, part), peer)
            gather_sums(peer, span, False)
            return c

        lax.fori_loop(1, st_n, grad_wait, 0)
        plow[:, span] = acc[:, span].astype(BF)

    scatter_first(1, plow, wkv, sp_part, sp_pair, sto_pair)

    def wkey_step(t, c):
        dwp[pl.ds(pl.multiple_of(t * chunk, chunk), chunk), :] = dot(
            rows[t], plow[:, :cols], TN
        ).astype(BF)
        return c

    lax.fori_loop(0, tp_n, wkey_step, 0)
    share = model // st_n

    def part_of(s):
        return dwp.at[pl.ds(pl.multiple_of(s * share, share), share), :]

    def wkey_send(d, c):
        peer = far_peer(d)
        z_copy(3, part_of(peer), dwr.at[st], peer).start()
        return c

    lax.fori_loop(1, st_n, wkey_send, 0)
    scatter_second(1, plow, wkv, sp_part, sp_pair, sp_part, sp_recv, sto_pair)
    scatter_last(0, tp_part, tp_pair, tp_part, tp_recv, tok_out)
    wkey_out[...] = part_of(st)[...].astype(F32)

    def wkey_wait(d, c):
        peer = (st + d) % st_n
        z_wait(3, part_of(peer), dwr.at[peer], peer)
        wkey_out[...] += dwr[peer].astype(F32)
        return c

    lax.fori_loop(1, st_n, wkey_wait, 0)
    scatter_last(1, sp_part, sp_pair, sp_part, sp_recv, store_out)

    for copy in across + [beside] + onward:
        copy.wait_send()

    def drain(d, c):
        peer = (st + d) % st_n
        z_copy(0, ask_ref.at[peer], ask_in.at[st], peer).wait_send()
        key_copy(peer).wait_send()
        value_copy(peer).wait_send()
        back_copy(2, vs_all, peer).wait_send()
        back_copy(5, ks, peer).wait_send()
        z_copy(3, part_of(peer), dwr.at[st], peer).wait_send()
        return c

    lax.fori_loop(1, st_n, drain, 0)
    for d in range(1, hi_n + 1):
        h = (hi + d) % hi_n
        pair_copy(0, tp_part, tp_pair, h).wait_send()
        pair_copy(1, sp_part, sp_pair, h).wait_send()
        if d < hi_n:
            cross(0, tp_part, tp_recv, h).wait_send()
            cross(1, sp_part, sp_recv, h).wait_send()


def local(pass_ids, store, queries, gate_pre, w_query, w_gate, w_key, w_value, d_mem):
    st_n = lax.axis_size("st")
    tp_n = lax.axis_size("tp")
    hi_n = tp_n // 2
    tok_rows, cols = queries.shape
    blocks = tok_rows // BLK
    passages, pass_len, chunk = store.shape
    model = w_key.shape[0]
    requests = blocks * PB
    depth = max(2, requests // st_n)
    pass_rows = passages * pass_len
    share = model // st_n

    ids = pass_ids.reshape(-1)
    owners = ids // passages
    within = ids % passages
    order = jnp.arange(requests, dtype=jnp.int32)
    earlier = (owners[None, :] == owners[:, None]) & (order[None, :] < order[:, None])
    rank = jnp.sum(earlier.astype(jnp.int32), axis=1)
    slots = jnp.stack([owners, rank])
    o_i = jnp.arange(st_n, dtype=jnp.int32)[:, None, None]
    k_i = jnp.arange(depth, dtype=jnp.int32)[None, :, None]
    match = (owners[None, None, :] == o_i) & (rank[None, None, :] == k_i)
    asked = jnp.max(jnp.where(match, within[None, None, :], -1), axis=2)
    req_of = jnp.max(jnp.where(match, order[None, None, :], 0), axis=2)
    hot_cols = depth * pass_len
    width = -(-hot_cols // 128) * 128
    lane = jnp.arange(width, dtype=jnp.int32)
    spread = jnp.repeat(asked, pass_len, axis=1)
    spread = jnp.pad(spread, ((0, 0), (0, width - hot_cols)), constant_values=-1)
    target = jnp.where(spread < 0, -1, spread * pass_len + lane[None, :] % pass_len)
    flat = jnp.pad(jnp.maximum(asked, 0), ((0, 0), (0, width - depth)))
    ask = jnp.concatenate(
        [target[:, None], flat[:, None], jnp.zeros((st_n, 6, width), jnp.int32)], axis=1
    )

    vmem = pl.BlockSpec(memory_space=pltpu.VMEM)
    smem = pl.BlockSpec(memory_space=pltpu.SMEM)
    hbm = pl.BlockSpec(memory_space=pl.ANY)
    V = pltpu.VMEM
    DMA = pltpu.SemaphoreType.DMA
    pair = 2 * cols
    tok_pair = tok_rows // tp_n
    sto_pair = pass_rows // tp_n
    d_tokens, d_store, d_wkey = pl.pallas_call(
        functools.partial(kernel, st_n, tp_n, depth, pass_len),
        out_shape=(
            jax.ShapeDtypeStruct((tok_pair, model), BF),
            jax.ShapeDtypeStruct((sto_pair, model), BF),
            jax.ShapeDtypeStruct((share, cols), F32),
        ),
        in_specs=[smem, smem, vmem] + [hbm] * 8,
        out_specs=(vmem, vmem, vmem),
        scratch_shapes=[
            V((tp_n, pass_rows, chunk), BF),
            V((model, pair), BF),
            V((model, pair), BF),
            V((tok_rows, cols), BF),
            V((tok_rows, cols), BF),
            V((tok_rows, cols), BF),
            V((pass_rows, pair), F32),
            V((passages, pass_len, pair), BF),
            V((st_n, 8, width), jnp.int32),
            pltpu.SMEM((st_n, 8, width), jnp.int32),
            V((st_n, depth, pass_len, pair), BF),
            V((st_n, depth, pass_len, cols), BF),
            V((st_n, depth, pass_len, cols), BF),
            V((st_n, depth, pass_len, pair), BF),
            V((cols // HD, tok_rows, PB * pass_len), F32),
            V((PB * pass_len, pair), BF),
            V((requests, pass_len, pair), BF),
            V((tok_rows, pair), BF),
            V((st_n, depth, pass_len, pair), BF),
            V((st_n, pass_rows, hot_cols), BF),
            V((pass_rows, pair), BF),
            V((model, cols), BF),
            V((st_n, share, cols), BF),
            V((tp_n, tok_pair, model), BF),
            V((hi_n, tok_pair, model), BF),
            V((hi_n, tok_pair, model), BF),
            V((tp_n, sto_pair, model), BF),
            V((hi_n, sto_pair, model), BF),
            V((hi_n, sto_pair, model), BF),
            DMA((9,)),
            DMA((3, hi_n)),
            DMA((tp_n,)),
            DMA((6, st_n)),
            DMA((6, st_n)),
            DMA((2, hi_n)),
            DMA((2, hi_n)),
            DMA((2, hi_n)),
            DMA((2, hi_n)),
        ],
        compiler_params=pltpu.CompilerParams(
            collective_id=0, has_side_effects=True, vmem_limit_bytes=67043328
        ),
    )(
        slots, req_of, ask, store.reshape(pass_rows, chunk),
        queries, gate_pre, w_query, w_gate, w_key, w_value, d_mem,
    )
    return d_tokens, d_store.reshape(passages // tp_n, pass_len, model), d_wkey


def solution(mesh):
    return jax.shard_map(
        local,
        mesh=mesh,
        in_specs=(
            P(("grp", "st"), None),
            P("st", None, "tp"),
            P(("grp", "st"), "tp"),
            P(("grp", "st"), "tp"),
            P(None, "tp"),
            P(None, "tp"),
            P(None, "tp"),
            P(None, "tp"),
            P(("grp", "st"), "tp"),
        ),
        out_specs=(
            P(("grp", "st", "tp"), None),
            P(("grp", "st", "tp"), None, None),
            P(("grp", "st"), "tp"),
        ),
        check_vma=False,
    )
```
